32 devices in a mesh: gr: 2 (over x), fs: 8 (over z, y), tp: 2 (over core).
Axes of the slice: x: 2, y: 2, z: 4, core: 2. Of those that a mesh axis runs over, the one named last changes fastest.
Arguments:
- prompt: bfloat16 [2048, 2048], P(('gr', 'tp'), 'fs'), may hold values from -2.5 to 2.5
- gain_pre: float32 [2048], P(('gr', 'fs')), may hold values from 0.1 to 1.9
- gate_pre: float32 [2048, 5632], P(('gr', 'fs'), 'tp'), may hold values from -6 to 6
- up_pre: float32 [2048, 5632], P(('gr', 'fs'), 'tp'), may hold values from -6 to 6
- down_pre: float32 [2048, 5632], P(('gr', 'fs'), 'tp'), may hold values from -6 to 6
- gain_post: float32 [2048], P(('gr', 'fs')), may hold values from 0.1 to 1.9
- gate_post: float32 [2048, 5632], P(('gr', 'fs'), 'tp'), may hold values from -6 to 6
- up_post: float32 [2048, 5632], P(('gr', 'fs'), 'tp'), may hold values from -6 to 6
- down_post: float32 [2048, 5632], P(('gr', 'fs'), 'tp'), may hold values from -6 to 6
Outputs:
- result: bfloat16 [2048, 2048], P(('gr', 'tp'), 'fs')
- gate_first: bfloat16 [5632, 2048], P('fs')
- up_first: bfloat16 [5632, 2048], P('fs')
- down_first: bfloat16 [5632, 2048], P('fs')
- gate_second: bfloat16 [5632, 2048], P('fs')
- up_second: bfloat16 [5632, 2048], P('fs')
- down_second: bfloat16 [5632, 2048], P('fs')
The draws below stay inside these ranges and needn't reach their ends.
All inputs are finite; a program needn't handle non-finite values.
Results may differ from the reference program's by a relative error of at most 0.028.
Values may be sent and summed in bfloat16 or wider, within the bound.
A program may use at most 128 MiB of HBM per device.

```python
import jax
import jax.numpy as jnp
from jax import lax

D = 2048
FF = 5632
TOKENS = 2048
N_FS = 8


def spiked(entries, key, source, target, parts, factor):
    def block_of(axis_at):
        return (jnp.arange(entries.shape[axis_at]) // (entries.shape[axis_at] // parts)).reshape((-1,) + (1,) * (entries.ndim - 1 - axis_at))

    near = jax.random.permutation(key, parts)[block_of(target)]
    far = (block_of(target) + parts // 2) % parts
    return jnp.where((block_of(source) == near) | (block_of(source) == far), factor * entries, entries)


def block_levels(stream_key, dims, split, smallest, largest):
    factor_of = 1.0
    for axis_at, blocks in split:
        steps = jax.random.uniform(jax.random.fold_in(jax.random.fold_in(stream_key, 6), axis_at), (blocks,), jnp.float32, smallest / len(split), largest / len(split))
        factor_of = factor_of * jnp.repeat(jnp.exp(steps), dims[axis_at] // blocks).reshape((-1,) + (1,) * (len(dims) - 1 - axis_at))
    return factor_of


def gaussian(stream_key, extent, deviation, reach, cuts=(), held_as=jnp.bfloat16):
    array = deviation * jax.random.normal(stream_key, extent, jnp.float32)
    if cuts:
        array = array * block_levels(stream_key, extent, cuts, -0.22, 0.18)
    return jnp.clip(array, -reach, reach).astype(held_as)


def heavy_noise(rng, dims, deviation, reach, cuts, heavy, held_as=jnp.bfloat16):
    entries = deviation * jax.random.normal(rng, dims, jnp.float32)
    if cuts:
        entries = entries * block_levels(rng, dims, cuts, -0.22, 0.18)
    return jnp.clip(spiked(entries, jax.random.fold_in(rng, 3), *heavy), -reach, reach).astype(held_as)


def setup_inputs(seed: int = 0) -> dict:
    keys = jax.random.split(jax.random.key(seed), 10)
    return {
        "prompt": gaussian(keys[0], (TOKENS, D), 0.3, 2.5, ((0, 4), (1, 8))),
        "gain_pre": jnp.clip(1.0 + 0.18 * jax.random.normal(keys[1], (D,), jnp.float32), 0.1, 1.9),
        "gate_pre": gaussian(keys[2], (D, FF), 1.0, 6.0, ((0, 16), (1, 2)), jnp.float32),
        "up_pre": gaussian(keys[3], (D, FF), 1.0, 6.0, ((0, 16), (1, 2)), jnp.float32),
        "down_pre": heavy_noise(keys[4], (D, FF), 1.0, 6.0, ((0, 16), (1, 2)), (1, 0, 16, 2.0), jnp.float32),
        "gain_post": jnp.clip(1.0 + 0.18 * jax.random.normal(keys[5], (D,), jnp.float32), 0.1, 1.9),
        "gate_post": gaussian(keys[6], (D, FF), 1.0, 6.0, ((0, 16), (1, 2)), jnp.float32),
        "up_post": gaussian(keys[7], (D, FF), 1.0, 6.0, ((0, 16), (1, 2)), jnp.float32),
        "down_post": heavy_noise(keys[8], (D, FF), 1.0, 6.0, ((0, 16), (1, 2)), (1, 0, 16, 2.0), jnp.float32),
    }


norm_eps = 1e-06

def fold_gain(gain, matrix):
    return (gain[:, None] * matrix).astype(jnp.bfloat16).T

def half_step(tokens, w_gate, w_up, w_down):
    row_count = tokens.shape[0]
    widened = tokens.astype(jnp.float32)
    row_scale = lax.rsqrt(lax.optimization_barrier(jnp.mean(widened * widened, axis=1)) + norm_eps) * D ** (-0.5)
    gate_sum = jnp.dot(tokens, w_gate.T, preferred_element_type=jnp.float32) * row_scale[:, None]
    up_sum = jnp.dot(tokens, w_up.T, preferred_element_type=jnp.float32) * row_scale[:, None]
    hidden = (jax.nn.silu(gate_sum) * up_sum).astype(jnp.bfloat16)
    group_width = FF // N_FS
    hidden_blocks = jnp.transpose(hidden.reshape(row_count, N_FS, group_width), (1, 0, 2))
    down_blocks = w_down.reshape(N_FS, group_width, D)

    def add_block(running, pair):
        term = jnp.dot(pair[0], pair[1], preferred_element_type=jnp.float32)
        rounded = lax.optimization_barrier(term.astype(jnp.bfloat16))
        return (running + rounded.astype(jnp.float32), None)
    branch, _ = lax.scan(add_block, jnp.zeros((row_count, D), jnp.float32), (hidden_blocks, down_blocks))
    return (widened + 0.5 * FF ** (-0.5) * branch).astype(jnp.bfloat16)

def reference(prompt, gain_pre, gate_pre, up_pre, down_pre, gain_post, gate_post, up_post, down_post):
    gate_first = fold_gain(gain_pre, gate_pre)
    up_first = fold_gain(gain_pre, up_pre)
    down_first = down_pre.astype(jnp.bfloat16).T
    gate_second = fold_gain(gain_post, gate_post)
    up_second = fold_gain(gain_post, up_post)
    down_second = down_post.astype(jnp.bfloat16).T
    middle = half_step(prompt, gate_first, up_first, down_first)
    result = half_step(middle, gate_second, up_second, down_second)
    return (result, gate_first, up_first, down_first, gate_second, up_second, down_second)
```

```python
import functools

import jax
import jax.numpy as jnp
from jax import lax
from jax.experimental import pallas as pl
from jax.experimental.pallas import tpu as pltpu
from jax.sharding import PartitionSpec as P

MESH = pl.DeviceIdType.MESH
LANES = 128


def lanes_of(block, width):
    return pl.ds(pl.multiple_of(block * width, width), width)


class HandOver:
    def __init__(self, shards, sources, held, land, first, onward):
        self.n, self.half = shards, shards // 2
        self.sources, self.held = sources, held
        self.land, self.first, self.onward = land, first, onward
        self.g, self.f, self.t = lax.axis_index("gr"), lax.axis_index("fs"), lax.axis_index("tp")
        self.height = held[0].shape[0]

    def slot(self, m, column):
        return self.held[m].at[:, lanes_of(column, LANES)]

    def copy(self, m, column, source, send, target):
        return pltpu.make_async_remote_copy(
            src_ref=source,
            dst_ref=self.slot(m, column),
            send_sem=send,
            recv_sem=self.land.at[m, column],
            device_id=target,
            device_id_type=MESH,
        )

    def outgoing(self, m, k, act):
        home = lax.rem(self.f, 2)
        target = self.t * self.half + k
        column = self.g * self.n + self.f
        block = self.sources[m].at[pl.ds(k * self.height, self.height), :]
        stays = jnp.logical_and(target == self.f, home == self.t)

        @pl.when(jnp.logical_not(stays))
        def _():
            act(self.copy(m, column, block, self.first.at[m, k], (self.g, target, home)))

        return stays, column, block

    def send(self, m, k):
        stays, column, block = self.outgoing(m, k, lambda c: c.start())

        @pl.when(stays)
        def _():
            pltpu.make_async_copy(block, self.slot(m, column), self.land.at[m, column]).start()

    def arrived(self, m, column):
        slot = self.slot(m, column)
        pltpu.make_async_copy(slot, slot, self.land.at[m, column]).wait()

    def forward(self, m, i, column, which):
        target = (1 - self.g, self.f, self.t) if which == 0 else (self.g, self.f, 1 - self.t)
        return self.copy(m, column, self.slot(m, column), self.onward.at[m, which * self.half + i], target)

    def near(self, i):
        return self.g * self.n + 2 * i + self.t

    def far(self, i):
        return (1 - self.g) * self.n + 2 * i + self.t

    def relay_near(self, m, i):
        self.arrived(m, self.near(i))
        self.forward(m, i, self.near(i), 0).start()
        self.forward(m, i, self.near(i), 1).start()

    def relay_far(self, m, i):
        self.arrived(m, self.far(i))
        self.forward(m, i, self.far(i), 2).start()

    def settle(self, m):
        for group in range(2):
            for i in range(self.half):
                self.arrived(m, group * self.n + 2 * i + 1 - self.t)

    def drain(self, m):
        for k in range(self.half):
            self.outgoing(m, k, lambda c: c.wait_send())
        for i in range(self.half):
            self.forward(m, i, self.near(i), 0).wait_send()
            self.forward(m, i, self.near(i), 1).wait_send()
            self.forward(m, i, self.far(i), 2).wait_send()


def greet(shards):
    g, f, t = lax.axis_index("gr"), lax.axis_index("fs"), lax.axis_index("tp")
    barrier = pltpu.get_barrier_semaphore()
    for step in range(1, 2 * shards):
        place = lax.rem(2 * f + t + step, 2 * shards)
        pl.semaphore_signal(barrier, inc=1, device_id=(g, place // 2, lax.rem(place, 2)), device_id_type=MESH)
    pl.semaphore_signal(barrier, inc=1, device_id=(1 - g, f, t), device_id_type=MESH)
    return lambda: pl.semaphore_wait(barrier, 2 * shards)


class Tokens:
    def __init__(self, shards, step, x, gathered, gather_out, over_y, into_y, y_out, y_in, over_z, into_z, z_out, z_in):
        self.n, self.depth, self.step = shards, shards // 2, step
        self.x, self.gathered, self.gather_out = x.at[step], gathered, gather_out
        self.over_y, self.into_y, self.y_out, self.y_in = over_y, into_y, y_out, y_in
        self.over_z, self.into_z, self.z_out, self.z_in = over_z, into_z, z_out, z_in
        self.g, self.f, self.t = lax.axis_index("gr"), lax.axis_index("fs"), lax.axis_index("tp")
        self.z, self.y = self.f // 2, lax.rem(self.f, 2)
        self.width = over_y.shape[-1]
        self.sent = []

    def go(self, when, make):
        @pl.when(when)
        def _():
            make().start()

        self.sent.append((when, make))

    def copy(self, source, dest, send, recv, target):
        return pltpu.make_async_remote_copy(
            src_ref=source,
            dst_ref=dest,
            send_sem=send,
            recv_sem=recv,
            device_id=(self.g, target, self.t),
            device_id_type=MESH,
        )

    def piece(self, owner):
        return self.x.at[:, lanes_of(owner, self.width)]

    def hand_on(self, when, source, owner, sem, target):
        self.go(when, lambda: self.copy(source(), self.piece(owner), self.gather_out.at[self.step, sem], self.gathered.at[self.step, owner], target))

    def spread(self, own):
        self.hand_on(self.z < self.depth - 1, lambda: own, self.f, 0, self.f + 2)
        self.hand_on(self.z > 0, lambda: own, self.f, 1, self.f - 2)
        self.hand_on(self.z >= 0, lambda: own, self.f, 2, 2 * self.z + 1 - self.y)

    def came(self, owner):
        piece = self.piece(owner)
        pltpu.make_async_copy(piece, piece, self.gathered.at[self.step, owner]).wait()

    def pass_on(self, i):
        for side, sign in enumerate((-1, 1)):
            place = self.z + sign * (1 + i)
            owner = 2 * place + self.y
            there = jnp.logical_and(place >= 0, place < self.depth)
            further = jnp.logical_and(there, self.z < self.depth - 1 if sign < 0 else self.z > 0)
            sem = 3 + 4 * i + 2 * side

            @pl.when(there)
            def _(owner=owner):
                self.came(owner)

            self.hand_on(further, lambda owner=owner: self.piece(owner), owner, sem, self.f - 2 * sign)
            self.hand_on(there, lambda owner=owner: self.piece(owner), owner, sem + 1, 2 * self.z + 1 - self.y)

    def collect(self):
        for i in range(self.depth):
            self.came(2 * i + 1 - self.y)

    def activate(self, w_gate, w_up, hidden, features):
        rows = self.x.shape[0]
        chunk = rows // 2

        @pl.loop(0, 2)
        def _(c):
            span = pl.ds(pl.multiple_of(c * chunk, chunk), chunk)
            tokens = self.x[span, :]
            widened = tokens.astype(jnp.float32)
            squares = jnp.sum(widened * widened, axis=1, keepdims=True)
            scale = lax.rsqrt(squares / features + norm_eps) * features ** (-0.5)
            dims = (((1,), (1,)), ((), ()))
            gate = lax.dot_general(tokens, w_gate[...], dims, preferred_element_type=jnp.float32) * scale
            up = lax.dot_general(tokens, w_up[...], dims, preferred_element_type=jnp.float32) * scale
            hidden[span, :] = (gate / (1.0 + jnp.exp(-gate)) * up).astype(jnp.bfloat16)

    def term(self, hidden, w_down, owner):
        return jnp.dot(hidden[...], w_down[:, lanes_of(owner, self.width)], preferred_element_type=jnp.float32)

    def place(self, k):
        n = self.depth
        low = self.z < n // 2
        z = jnp.where(low, self.z, n - 1 - self.z)
        lead = n - 1 - 2 * z
        j = k - lead
        nearby = z + (1 - 2 * lax.rem(jnp.maximum(j, 0), 2)) * (z - jnp.maximum(j, 0) // 2)
        found = jnp.where(j < 0, n - 1 - k, nearby)
        return jnp.where(low, found, n - 1 - found)

    def swap(self, hidden, w_down, k):
        s = self.step
        self.over_y[s, k] = self.term(hidden, w_down, 2 * self.place(k) + 1 - self.y).astype(jnp.bfloat16)
        self.go(
            self.z >= 0,
            lambda: self.copy(self.over_y.at[s, k], self.into_y.at[s, k], self.y_out.at[s, k], self.y_in.at[s, k], 2 * self.z + 1 - self.y),
        )

    def gather_term(self, hidden, w_down, own, k):
        s = self.step
        own[k] = self.term(hidden, w_down, 2 * self.place(k) + self.y)

    def reduce(self, own, k):
        s = self.step
        place = self.place(k)
        up = place > self.z
        side = jnp.where(up, 0, 1)
        inner = jnp.where(up, self.z, self.depth - 1 - self.z) > 0
        self.wait(self.into_y.at[s, k], self.y_in.at[s, k])

        @pl.when(inner)
        def _():
            self.wait(self.into_z.at[s, side, place], self.z_in.at[s, side, place])
            total = own[k] + self.into_y[s, k].astype(jnp.float32) + self.into_z[s, side, place].astype(jnp.float32)
            self.over_z[s, k] = total.astype(jnp.bfloat16)

        @pl.when(jnp.logical_not(inner))
        def _():
            self.over_z[s, k] = (own[k] + self.into_y[s, k].astype(jnp.float32)).astype(jnp.bfloat16)

        self.go(
            self.z >= 0,
            lambda: self.copy(
                self.over_z.at[s, k],
                self.into_z.at[s, side, place],
                self.z_out.at[s, k],
                self.z_in.at[s, side, place],
                self.f + 2 - 4 * side,
            ),
        )

    def wait(self, landed, sem):
        pltpu.make_async_copy(landed, landed, sem).wait()

    def finish(self, own, units):
        s, k = self.step, self.depth - 1
        self.wait(self.into_y.at[s, k], self.y_in.at[s, k])
        own[k] += self.into_y[s, k].astype(jnp.float32)
        for side in range(2):
            inner = self.z > 0 if side == 0 else self.z < self.depth - 1

            @pl.when(inner)
            def _(side=side):
                self.wait(self.into_z.at[s, side, self.z], self.z_in.at[s, side, self.z])
                own[k] += self.into_z[s, side, self.z].astype(jnp.float32)

        before = self.x[:, lanes_of(self.f, self.width)].astype(jnp.float32)
        return (before + 0.5 * units ** (-0.5) * own[k]).astype(jnp.bfloat16)

    def drain(self):
        for when, make in self.sent:

            @pl.when(when)
            def _(make=make):
                make().wait_send()


def whole_kernel(shards, features, units, *refs):
    prompt, gains, trained, result, held = refs[0], refs[1:3], refs[3:9], refs[9], refs[10:16]
    land, first, onward, x, hidden, own, middle = refs[16:23]
    traffic, alone, raw, turned, loaded = refs[23:33], refs[33], refs[34], refs[35], refs[36]
    sources = [turned.at[m] for m in range(6)]
    loads = [pltpu.make_async_copy(trained[m], raw.at[m], loaded.at[m]) for m in range(6)]
    moves = HandOver(shards, sources, held, land, first, onward)
    steps = [Tokens(shards, s, x, *traffic) for s in range(2)]
    half = shards // 2

    def prepare(m):
        loads[m].wait()
        for c in range(raw.shape[2] // LANES):
            span = pl.ds(c * LANES, LANES)
            block = raw[m, :, span].T
            if m % 3 < 2:
                block = block * gains[m // 3][...]
            turned[m, span, :] = block.astype(jnp.bfloat16)

    def send(m):
        for k in range(half):
            moves.send(m, k)

    def near(m):
        for i in range(half):
            moves.relay_near(m, i)

    def far(m):
        for i in range(half):
            moves.relay_far(m, i)

    for load in loads:
        load.start()
    ready = greet(shards)
    prepare(0)
    ready()
    start = pltpu.make_async_copy(prompt, steps[0].piece(steps[0].f), alone.at[0])
    start.start()
    steps[0].spread(prompt)
    send(0)
    prepare(1)
    prepare(2)
    prepare(3)
    prepare(4)
    prepare(5)
    steps[0].pass_on(0)
    send(1)
    near(0)
    send(2)
    steps[0].pass_on(1)
    for i in range(half):
        moves.relay_far(0, i)
        moves.relay_near(1, i)
    send(3)
    steps[0].pass_on(2)
    for i in range(half):
        moves.relay_near(2, i)
        moves.relay_far(1, i)
    start.wait()
    steps[0].collect()
    for m in range(2):
        moves.settle(m)
    steps[0].activate(held[0], held[1], hidden, features)
    far(2)
    moves.settle(2)
    for k in range(4):
        steps[0].swap(hidden, held[2], k)
    for k in range(4):
        steps[0].gather_term(hidden, held[2], own, k)
    moves.send(4, 0)
    near(3)
    steps[0].reduce(own, 0)
    moves.send(4, 1)
    steps[0].reduce(own, 1)
    moves.send(4, 2)
    moves.send(4, 3)
    steps[0].reduce(own, 2)
    moves.send(5, 0)
    moves.send(5, 1)
    tokens = steps[0].finish(own, units)
    middle[...] = tokens
    x[1, :, lanes_of(steps[1].f, steps[1].width)] = tokens
    steps[1].spread(middle)
    moves.send(5, 2)
    far(3)
    steps[1].pass_on(0)
    moves.send(5, 3)
    near(4)
    steps[1].pass_on(1)
    far(4)
    steps[1].pass_on(2)
    near(5)
    steps[1].collect()
    for m in range(3, 5):
        moves.settle(m)
    steps[1].activate(held[3], held[4], hidden, features)
    far(5)
    moves.settle(5)
    for k in range(4):
        steps[1].swap(hidden, held[5], k)
    for k in range(4):
        steps[1].gather_term(hidden, held[5], own, k)
    steps[1].reduce(own, 0)
    steps[1].reduce(own, 1)
    steps[1].reduce(own, 2)
    result[...] = steps[1].finish(own, units)
    for m in range(6):
        moves.drain(m)
    for step in steps:
        step.drain()


def whole(prompt, gains, trained, shards):
    units = trained[0].shape[1] * lax.axis_size("tp")
    height = units // shards
    features = LANES * lax.axis_size("gr") * shards
    rows, width = prompt.shape
    depth = shards // 2
    any_space = pl.BlockSpec(memory_space=pl.ANY)
    vmem = pl.BlockSpec(memory_space=pltpu.VMEM)
    return pl.pallas_call(
        functools.partial(whole_kernel, shards, features, units),
        out_shape=[pltpu.VMEM(prompt.shape, jnp.bfloat16)] + [pltpu.VMEM((height, features), jnp.bfloat16)] * 6,
        in_specs=[any_space] + [vmem] * 2 + [any_space] * 6,
        out_specs=[vmem] * 7,
        scratch_shapes=[
            pltpu.SemaphoreType.DMA((6, 2 * shards)),
            pltpu.SemaphoreType.DMA((6, shards // 2)),
            pltpu.SemaphoreType.DMA((6, 3 * shards // 2)),
            pltpu.VMEM((2, rows, features), jnp.bfloat16),
            pltpu.VMEM((rows, height), jnp.bfloat16),
            pltpu.VMEM((depth, rows, width), jnp.float32),
            pltpu.VMEM((rows, width), jnp.bfloat16),
            pltpu.SemaphoreType.DMA((2, shards)),
            pltpu.SemaphoreType.DMA((2, 4 * depth)),
            pltpu.VMEM((2, depth, rows, width), jnp.bfloat16),
            pltpu.VMEM((2, depth, rows, width), jnp.bfloat16),
            pltpu.SemaphoreType.DMA((2, depth)),
            pltpu.SemaphoreType.DMA((2, depth)),
            pltpu.VMEM((2, depth, rows, width), jnp.bfloat16),
            pltpu.VMEM((2, 2, depth, rows, width), jnp.bfloat16),
            pltpu.SemaphoreType.DMA((2, depth)),
            pltpu.SemaphoreType.DMA((2, 2, depth)),
            pltpu.SemaphoreType.DMA((1,)),
            pltpu.VMEM((6,) + trained[0].shape, jnp.float32),
            pltpu.VMEM((6, trained[0].shape[1], LANES), jnp.bfloat16),
            pltpu.SemaphoreType.DMA((6,)),
        ],
        compiler_params=pltpu.CompilerParams(collective_id=0, has_side_effects=True, vmem_limit_bytes=40 << 20),
    )(prompt, *gains, *trained)


D = 2048
FF = 5632


norm_eps = 1e-06


def add_products(columns_in, w_gate, w_up):
    widened = columns_in.astype(jnp.float32)
    dims = (((1,), (1,)), ((), ()))
    return (
        lax.dot_general(columns_in, w_gate, dims, preferred_element_type=jnp.float32),
        lax.dot_general(columns_in, w_up, dims, preferred_element_type=jnp.float32),
        jnp.sum(widened * widened, axis=1),
    )


def half_step(tokens, w_gate, w_up, w_down):
    gate_sum, up_sum, squares = add_products(
        lax.all_gather(tokens, "fs", axis=1, tiled=True), w_gate, w_up
    )
    row_scale = (lax.rsqrt(squares / D + norm_eps) * D ** (-0.5))[:, None]
    hidden = (jax.nn.silu(gate_sum * row_scale) * (up_sum * row_scale)).astype(jnp.bfloat16)
    partial_value = jnp.dot(hidden, w_down, preferred_element_type=jnp.float32)
    summed = lax.psum_scatter(
        partial_value.astype(jnp.bfloat16), "fs", scatter_dimension=1, tiled=True
    ).astype(jnp.float32)
    return (tokens.astype(jnp.float32) + 0.5 * FF ** (-0.5) * summed).astype(jnp.bfloat16)


def restore_rows(matrix, groups, shards, lanes):
    row_total, col_total = matrix.shape
    sub_rows = row_total // (groups * shards * lanes)
    shaped = matrix.reshape(groups, lanes, shards, sub_rows, col_total)
    return jnp.transpose(shaped, (0, 2, 1, 3, 4)).reshape(row_total, col_total)


def relayout(matrices):
    crossed = (
        lax.all_to_all(
            lax.all_to_all(matrices[0], "tp", split_axis=0, concat_axis=1, tiled=True),
            "fs",
            split_axis=1,
            concat_axis=0,
            tiled=True,
        ),
        lax.all_to_all(
            lax.all_to_all(matrices[1], "tp", split_axis=0, concat_axis=1, tiled=True),
            "fs",
            split_axis=1,
            concat_axis=0,
            tiled=True,
        ),
        lax.all_to_all(
            lax.all_to_all(matrices[2], "tp", split_axis=0, concat_axis=1, tiled=True),
            "fs",
            split_axis=1,
            concat_axis=0,
            tiled=True,
        ),
        lax.all_to_all(
            lax.all_to_all(matrices[3], "tp", split_axis=0, concat_axis=1, tiled=True),
            "fs",
            split_axis=1,
            concat_axis=0,
            tiled=True,
        ),
        lax.all_to_all(
            lax.all_to_all(matrices[4], "tp", split_axis=0, concat_axis=1, tiled=True),
            "fs",
            split_axis=1,
            concat_axis=0,
            tiled=True,
        ),
        lax.all_to_all(
            lax.all_to_all(matrices[5], "tp", split_axis=0, concat_axis=1, tiled=True),
            "fs",
            split_axis=1,
            concat_axis=0,
            tiled=True,
        ),
    )
    gathered = (
        lax.all_gather(crossed[0], ("gr", "tp"), axis=0, tiled=True),
        lax.all_gather(crossed[1], ("gr", "tp"), axis=0, tiled=True),
        lax.all_gather(crossed[2], ("gr", "tp"), axis=0, tiled=True),
        lax.all_gather(crossed[3], ("gr", "tp"), axis=0, tiled=True),
        lax.all_gather(crossed[4], ("gr", "tp"), axis=0, tiled=True),
        lax.all_gather(crossed[5], ("gr", "tp"), axis=0, tiled=True),
    )
    groups = lax.axis_size("gr")
    shards = lax.axis_size("fs")
    lanes = lax.axis_size("tp")
    return tuple((restore_rows(matrix, groups, shards, lanes).T for matrix in gathered))


def direct_fits(token_shape, shape):
    shards = lax.axis_size("fs")
    units = shape[1] * lax.axis_size("tp")
    whole_rows = shape[0] == LANES and shape[1] % LANES == 0 and units % (16 * shards) == 0
    whole_tokens = token_shape[0] % 32 == 0 and token_shape[1] % LANES == 0
    pairs = shards % 4 == 0 and lax.axis_size("gr") == 2 and lax.axis_size("tp") == 2
    return whole_rows and whole_tokens and pairs


def local(prompt, gain_pre, gate_pre, up_pre, down_pre, gain_post, gate_post, up_post, down_post):
    rounded = (
        (gain_pre[:, None] * gate_pre).astype(jnp.bfloat16),
        (gain_pre[:, None] * up_pre).astype(jnp.bfloat16),
        down_pre.astype(jnp.bfloat16),
        (gain_post[:, None] * gate_post).astype(jnp.bfloat16),
        (gain_post[:, None] * up_post).astype(jnp.bfloat16),
        down_post.astype(jnp.bfloat16),
    )
    if direct_fits(prompt.shape, gate_pre.shape):
        trained = (gate_pre, up_pre, down_pre, gate_post, up_post, down_post)
        gains = (gain_pre[None, :], gain_post[None, :])
        return tuple(whole(prompt, gains, trained, lax.axis_size("fs")))
    served = relayout(rounded)
    middle = half_step(prompt, served[0], served[1], served[2])
    result = half_step(middle, served[3], served[4], served[5])
    return (result, served[0], served[1], served[2], served[3], served[4], served[5])


def solution(mesh):
    placed = (
        P(("gr", "tp"), "fs"),
        P(("gr", "fs")),
        P(("gr", "fs"), "tp"),
        P(("gr", "fs"), "tp"),
        P(("gr", "fs"), "tp"),
        P(("gr", "fs")),
        P(("gr", "fs"), "tp"),
        P(("gr", "fs"), "tp"),
        P(("gr", "fs"), "tp"),
    )
    return jax.shard_map(
        local,
        mesh=mesh,
        in_specs=placed,
        out_specs=(
            P(("gr", "tp"), "fs"),
            P("fs", None),
            P("fs", None),
            P("fs", None),
            P("fs", None),
            P("fs", None),
            P("fs", None),
        ),
        check_vma=False,
    )
```

```python
import functools

import jax
import jax.numpy as jnp
from jax import lax
from jax.experimental import pallas as pl
from jax.experimental.pallas import tpu as pltpu
from jax.sharding import PartitionSpec as P

MESH = pl.DeviceIdType.MESH
LANES = 128


def lanes_of(block, width):
    return pl.ds(pl.multiple_of(block * width, width), width)


def place_of(count, here, k):
    low = here < count // 2
    z = jnp.where(low, here, count - 1 - here)
    j = k - (count - 1 - 2 * z)
    late = jnp.maximum(j, 0)
    nearby = z + (1 - 2 * lax.rem(late, 2)) * (z - late // 2)
    found = jnp.where(j < 0, count - 1 - k, nearby)
    return jnp.where(low, found, count - 1 - found)


class HandOver:
    def __init__(self, shards, sources, held, land, first, onward):
        self.n, self.half = shards, shards // 2
        self.sources, self.held = sources, held
        self.land, self.first, self.onward = land, first, onward
        self.g, self.f, self.t = lax.axis_index("gr"), lax.axis_index("fs"), lax.axis_index("tp")
        self.height = held[0].shape[0]

    def slot(self, m, column):
        return self.held[m].at[:, lanes_of(column, LANES)]

    def copy(self, m, column, source, send, target):
        return pltpu.make_async_remote_copy(
            src_ref=source,
            dst_ref=self.slot(m, column),
            send_sem=send,
            recv_sem=self.land.at[m, column],
            device_id=target,
            device_id_type=MESH,
        )

    def outgoing(self, m, k, act):
        home = lax.rem(self.f, 2)
        target = self.t * self.half + k
        column = self.g * self.n + self.f
        block = self.sources[m].at[pl.ds(pl.multiple_of(k * self.height, 16), self.height), :]
        stays = jnp.logical_and(target == self.f, home == self.t)

        @pl.when(jnp.logical_not(stays))
        def _():
            act(self.copy(m, column, block, self.first.at[m, k], (self.g, target, home)))

        return stays, column, block

    def send(self, m, k):
        stays, column, block = self.outgoing(m, k, lambda c: c.start())

        @pl.when(stays)
        def _():
            pltpu.make_async_copy(block, self.slot(m, column), self.land.at[m, column]).start()

    def arrived(self, m, column):
        slot = self.slot(m, column)
        pltpu.make_async_copy(slot, slot, self.land.at[m, column]).wait()

    def forward(self, m, i, column, which):
        target = (1 - self.g, self.f, self.t) if which == 0 else (self.g, self.f, 1 - self.t)
        return self.copy(m, column, self.slot(m, column), self.onward.at[m, which * self.half + i], target)

    def near(self, i):
        return self.g * self.n + 2 * i + self.t

    def far(self, i):
        return (1 - self.g) * self.n + 2 * i + self.t

    def relay_near(self, m, j):
        i = place_of(self.half, self.f // 2, self.half - 1 - j)
        self.arrived(m, self.near(i))
        self.forward(m, i, self.near(i), 0).start()
        self.forward(m, i, self.near(i), 1).start()

    def relay_far(self, m, j):
        i = place_of(self.half, self.f // 2, self.half - 1 - j)
        self.arrived(m, self.far(i))
        self.forward(m, i, self.far(i), 2).start()

    def settle(self, m):
        for group in range(2):
            for i in range(self.half):
                self.arrived(m, group * self.n + 2 * i + 1 - self.t)

    def drain(self, m):
        for k in range(self.half):
            self.outgoing(m, k, lambda c: c.wait_send())
        for i in range(self.half):
            self.forward(m, i, self.near(i), 0).wait_send()
            self.forward(m, i, self.near(i), 1).wait_send()
            self.forward(m, i, self.far(i), 2).wait_send()


def greet(shards):
    g, f, t = lax.axis_index("gr"), lax.axis_index("fs"), lax.axis_index("tp")
    barrier = pltpu.get_barrier_semaphore()
    for step in range(1, 2 * shards):
        place = lax.rem(2 * f + t + step, 2 * shards)
        pl.semaphore_signal(barrier, inc=1, device_id=(g, place // 2, lax.rem(place, 2)), device_id_type=MESH)
    pl.semaphore_signal(barrier, inc=1, device_id=(1 - g, f, t), device_id_type=MESH)
    return lambda: pl.semaphore_wait(barrier, 2 * shards)


CHUNKS = 4


class Tokens:
    def __init__(self, shards, step, x, gathered, gather_out, over_y, into_y, y_out, y_in, over_z, into_z, z_out, z_in):
        self.n, self.depth = shards, shards // 2
        self.x, self.gathered, self.gather_out = x.at[step], gathered.at[step], gather_out.at[step]
        self.over_y, self.into_y, self.y_out, self.y_in = over_y.at[step], into_y.at[step], y_out.at[step], y_in.at[step]
        self.over_z, self.into_z, self.z_out, self.z_in = over_z.at[step], into_z.at[step], z_out.at[step], z_in.at[step]
        self.g, self.f, self.t = lax.axis_index("gr"), lax.axis_index("fs"), lax.axis_index("tp")
        self.z, self.y = self.f // 2, lax.rem(self.f, 2)
        self.width = over_y.shape[-1]
        self.rows = x.shape[1] // CHUNKS
        self.sent = []

    def span(self, c):
        return pl.ds(c * self.rows, self.rows)

    def go(self, when, make):
        @pl.when(when)
        def _():
            make().start()

        self.sent.append((when, make))

    def copy(self, source, dest, send, recv, target):
        return pltpu.make_async_remote_copy(
            src_ref=source,
            dst_ref=dest,
            send_sem=send,
            recv_sem=recv,
            device_id=(self.g, target, self.t),
            device_id_type=MESH,
        )

    def piece(self, owner, c):
        return self.x.at[self.span(c), lanes_of(owner, self.width)]

    def hand_on(self, when, source, owner, sem, target, c):
        self.go(when, lambda: self.copy(source(), self.piece(owner, c), self.gather_out.at[c, sem], self.gathered.at[c, owner], target))

    def spread(self, own, c):
        source = own.at[self.span(c), :]
        self.hand_on(self.z < self.depth - 1, lambda: source, self.f, 0, self.f + 2, c)
        self.hand_on(self.z > 0, lambda: source, self.f, 1, self.f - 2, c)
        self.hand_on(self.z >= 0, lambda: source, self.f, 2, 2 * self.z + 1 - self.y, c)

    def came(self, owner, c):
        piece = self.piece(owner, c)
        pltpu.make_async_copy(piece, piece, self.gathered.at[c, owner]).wait()

    def pass_on(self, i, c):
        for side, sign in enumerate((-1, 1)):
            place = self.z + sign * (1 + i)
            owner = 2 * place + self.y
            there = jnp.logical_and(place >= 0, place < self.depth)
            further = jnp.logical_and(there, self.z < self.depth - 1 if sign < 0 else self.z > 0)
            sem = 3 + 4 * i + 2 * side

            @pl.when(there)
            def _(owner=owner):
                self.came(owner, c)

            self.hand_on(further, lambda owner=owner: self.piece(owner, c), owner, sem, self.f - 2 * sign, c)
            self.hand_on(there, lambda owner=owner: self.piece(owner, c), owner, sem + 1, 2 * self.z + 1 - self.y, c)

    def collect(self):
        for i in range(self.depth):
            for c in range(CHUNKS):
                self.came(2 * i + 1 - self.y, c)

    def activate(self, w_gate, w_up, hidden, features):
        rows = self.x.shape[0]
        chunk = rows // 2

        @pl.loop(0, 2)
        def _(c):
            span = pl.ds(pl.multiple_of(c * chunk, chunk), chunk)
            tokens = self.x[span, :]
            widened = tokens.astype(jnp.float32)
            squares = jnp.sum(widened * widened, axis=1, keepdims=True)
            scale = lax.rsqrt(squares / features + norm_eps) * features ** (-0.5)
            dims = (((1,), (1,)), ((), ()))
            gate = lax.dot_general(tokens, w_gate[...], dims, preferred_element_type=jnp.float32) * scale
            up = lax.dot_general(tokens, w_up[...], dims, preferred_element_type=jnp.float32) * scale
            hidden[span, :] = (gate / (1.0 + jnp.exp(-gate)) * up).astype(jnp.bfloat16)

    def term(self, hidden, w_down, owner):
        return jnp.dot(hidden[...], w_down[:, lanes_of(owner, self.width)], preferred_element_type=jnp.float32)

    def place(self, k):
        return place_of(self.depth, self.z, k)

    def swap(self, hidden, w_down, k):
        self.over_y[k] = self.term(hidden, w_down, 2 * self.place(k) + 1 - self.y).astype(jnp.bfloat16)
        for c in range(CHUNKS):
            part = (k, self.span(c))
            self.go(
                self.z >= 0,
                lambda c=c, part=part: self.copy(self.over_y.at[part], self.into_y.at[part], self.y_out.at[c, k], self.y_in.at[c, k], 2 * self.z + 1 - self.y),
            )

    def gather_term(self, hidden, w_down, own, k):
        own[k] = self.term(hidden, w_down, 2 * self.place(k) + self.y)

    def reduce(self, own, k, c):
        place = self.place(k)
        up = place > self.z
        side = jnp.where(up, 0, 1)
        inner = jnp.where(up, self.z, self.depth - 1 - self.z) > 0
        part = (k, self.span(c))
        passed = (side, place, self.span(c))
        self.wait(self.into_y.at[part], self.y_in.at[c, k])

        @pl.when(inner)
        def _():
            self.wait(self.into_z.at[passed], self.z_in.at[c, side, place])
            total = own[part] + self.into_y[part].astype(jnp.float32) + self.into_z[passed].astype(jnp.float32)
            self.over_z[part] = total.astype(jnp.bfloat16)

        @pl.when(jnp.logical_not(inner))
        def _():
            self.over_z[part] = (own[part] + self.into_y[part].astype(jnp.float32)).astype(jnp.bfloat16)

        self.go(
            self.z >= 0,
            lambda: self.copy(
                self.over_z.at[part],
                self.into_z.at[passed],
                self.z_out.at[c, k],
                self.z_in.at[c, side, place],
                self.f + 2 - 4 * side,
            ),
        )

    def wait(self, landed, sem):
        pltpu.make_async_copy(landed, landed, sem).wait()

    def finish(self, own, units, c):
        k = self.depth - 1
        part = (k, self.span(c))
        self.wait(self.into_y.at[part], self.y_in.at[c, k])
        own[part] += self.into_y[part].astype(jnp.float32)
        for side in range(2):
            inner = self.z > 0 if side == 0 else self.z < self.depth - 1

            @pl.when(inner)
            def _(side=side):
                passed = (side, self.z, self.span(c))
                self.wait(self.into_z.at[passed], self.z_in.at[c, side, self.z])
                own[part] += self.into_z[passed].astype(jnp.float32)

        before = self.x[self.span(c), lanes_of(self.f, self.width)].astype(jnp.float32)
        return (before + 0.5 * units ** (-0.5) * own[part]).astype(jnp.bfloat16)

    def drain(self):
        for when, make in self.sent:

            @pl.when(when)
            def _(make=make):
                make().wait_send()


def whole_kernel(shards, features, units, *refs):
    prompt, gains, trained, result, held = refs[0], refs[1:3], refs[3:9], refs[9], refs[10:16]
    land, first, onward, x, hidden, own, middle = refs[16:23]
    traffic, alone, raw, turned, loaded = refs[23:33], refs[33], refs[34], refs[35], refs[36]
    sources = [turned.at[m] for m in range(6)]
    loads = [pltpu.make_async_copy(trained[m], raw.at[m], loaded.at[m]) for m in range(6)]
    moves = HandOver(shards, sources, held, land, first, onward)
    half = shards // 2
    tokens = [Tokens(shards, step, x, *traffic) for step in range(2)]

    def prepare(m):
        loads[m].wait()
        for c in range(raw.shape[2] // LANES):
            span = pl.ds(c * LANES, LANES)
            block = raw[m, :, span].T
            if m % 3 < 2:
                block = block * gains[m // 3][...]
            turned[m, span, :] = block.astype(jnp.bfloat16)

    def send(m):
        for k in range(half):
            moves.send(m, k)

    row = lax.rem(moves.f, 2)
    turning = row != moves.t

    def send_turning(m):
        for j in range(half // 2):
            moves.send(m, 2 * j + 1 - row)

    def send_straight(m):
        for j in range(half // 2):
            moves.send(m, 2 * j + row)

    def near_if(m, turned_row):
        @pl.when(turning if turned_row else jnp.logical_not(turning))
        def _():
            for i in range(half):
                moves.relay_near(m, i)

    def far_if(m, turned_row):
        @pl.when(turning if turned_row else jnp.logical_not(turning))
        def _():
            for i in range(half):
                moves.relay_far(m, i)

    def spread(step, own_tokens):
        for c in range(CHUNKS):
            tokens[step].spread(own_tokens, c)

    def pass_on(step, i):
        for c in range(CHUNKS):
            tokens[step].pass_on(i, c)

    def activate(step):
        tokens[step].activate(held[3 * step], held[3 * step + 1], hidden, features)

    def swap(step):
        for k in range(half):
            tokens[step].swap(hidden, held[3 * step + 2], k)

    def terms(step):
        for k in range(half):
            tokens[step].gather_term(hidden, held[3 * step + 2], own, k)

    def reduce(step, k):
        for c in range(CHUNKS):
            tokens[step].reduce(own, k, c)

    def hand_back():
        for c in range(CHUNKS):
            span = tokens[0].span(c)
            done = tokens[0].finish(own, units, c)
            middle[span, :] = done
            x[1, span, lanes_of(tokens[1].f, tokens[1].width)] = done
            tokens[1].spread(middle, c)

    def deliver():
        for c in range(CHUNKS):
            result[tokens[1].span(c), :] = tokens[1].finish(own, units, c)

    for load in loads:
        load.start()
    ready = greet(shards)
    prepare(0)
    ready()
    start = pltpu.make_async_copy(prompt, x.at[0, :, lanes_of(moves.f, prompt.shape[1])], alone.at[0])
    start.start()
    spread(0, prompt)
    moves.send(0, 0)
    moves.send(0, 1)
    moves.send(0, 2)
    moves.send(0, 3)
    prepare(1)
    prepare(2)
    prepare(3)
    prepare(4)
    prepare(5)
    pass_on(0, 0)
    moves.send(1, 0)
    moves.send(1, 1)
    moves.relay_near(0, 0)
    moves.relay_near(0, 1)
    moves.relay_near(0, 2)
    pass_on(0, 1)
    moves.relay_near(0, 3)
    moves.send(1, 2)
    moves.send(1, 3)
    moves.relay_near(1, 0)
    moves.relay_near(1, 1)
    moves.relay_near(1, 2)
    moves.send(2, 0)
    moves.send(2, 1)
    pass_on(0, 2)
    moves.relay_near(1, 3)
    moves.send(2, 2)
    moves.send(2, 3)
    moves.relay_far(0, 0)
    moves.relay_far(0, 1)
    moves.relay_far(0, 2)
    moves.relay_far(0, 3)
    moves.relay_near(2, 0)
    moves.relay_near(2, 1)
    moves.relay_near(2, 2)
    moves.send(3, 0)
    moves.send(3, 1)
    moves.send(3, 2)
    moves.send(3, 3)
    moves.relay_near(2, 3)
    moves.relay_far(1, 0)
    moves.relay_far(1, 1)
    moves.relay_far(1, 2)
    moves.relay_far(1, 3)
    start.wait()
    tokens[0].collect()
    moves.settle(0)
    moves.settle(1)
    activate(0)
    moves.send(4, 0)
    moves.send(4, 1)
    moves.send(4, 2)
    moves.send(4, 3)
    moves.relay_far(2, 0)
    moves.relay_far(2, 1)
    moves.relay_far(2, 2)
    moves.relay_far(2, 3)
    moves.settle(2)
    swap(0)
    terms(0)
    moves.send(5, 0)
    moves.send(5, 1)
    moves.send(5, 2)
    moves.send(5, 3)
    moves.relay_near(3, 0)
    moves.relay_near(3, 1)
    moves.relay_near(3, 2)
    moves.relay_near(3, 3)
    reduce(0, 0)
    reduce(0, 1)
    moves.relay_near(4, 0)
    moves.relay_near(4, 1)
    moves.relay_near(4, 2)
    moves.relay_near(4, 3)
    reduce(0, 2)
    hand_back()
    moves.relay_far(3, 0)
    moves.relay_far(3, 1)
    moves.relay_far(3, 2)
    moves.relay_far(3, 3)
    moves.relay_near(5, 0)
    moves.relay_near(5, 1)
    moves.relay_near(5, 2)
    moves.relay_near(5, 3)
    pass_on(1, 0)
    moves.relay_far(4, 0)
    moves.relay_far(4, 1)
    moves.relay_far(4, 2)
    moves.relay_far(4, 3)
    pass_on(1, 1)
    moves.relay_far(5, 0)
    moves.relay_far(5, 1)
    moves.relay_far(5, 2)
    moves.relay_far(5, 3)
    pass_on(1, 2)
    tokens[1].collect()
    moves.settle(3)
    moves.settle(4)
    activate(1)
    moves.settle(5)
    swap(1)
    terms(1)
    reduce(1, 0)
    reduce(1, 1)
    reduce(1, 2)
    deliver()
    for m in range(6):
        moves.drain(m)
    for part in tokens:
        part.drain()


def write_kernel(count, *refs):
    sources, outs, written = refs[:count], refs[count : 2 * count], refs[2 * count]
    copies = [pltpu.make_async_copy(sources[i], outs[i], written.at[i]) for i in range(count)]
    for copy in copies:
        copy.start()
    for copy in copies:
        copy.wait()


def write_out(arrays):
    count = len(arrays)
    return pl.pallas_call(
        functools.partial(write_kernel, count),
        out_shape=[jax.ShapeDtypeStruct(a.shape, a.dtype) for a in arrays],
        in_specs=[pl.BlockSpec(memory_space=pltpu.VMEM)] * count,
        out_specs=[pl.BlockSpec(memory_space=pl.ANY)] * count,
        scratch_shapes=[pltpu.SemaphoreType.DMA((count,))],
        compiler_params=pltpu.CompilerParams(vmem_limit_bytes=1 << 20),
    )(*[pltpu.with_memory_space_constraint(a, pltpu.VMEM) for a in arrays])


def whole(prompt, gains, trained, shards):
    units = trained[0].shape[1] * lax.axis_size("tp")
    height = units // shards
    features = LANES * lax.axis_size("gr") * shards
    rows, width = prompt.shape
    depth = shards // 2
    any_space = pl.BlockSpec(memory_space=pl.ANY)
    vmem = pl.BlockSpec(memory_space=pltpu.VMEM)
    outs = pl.pallas_call(
        functools.partial(whole_kernel, shards, features, units),
        out_shape=[pltpu.VMEM(prompt.shape, jnp.bfloat16)] + [pltpu.VMEM((height, features), jnp.bfloat16)] * 6,
        in_specs=[any_space] + [vmem] * 2 + [any_space] * 6,
        out_specs=[vmem] * 7,
        scratch_shapes=[
            pltpu.SemaphoreType.DMA((6, 2 * shards)),
            pltpu.SemaphoreType.DMA((6, shards // 2)),
            pltpu.SemaphoreType.DMA((6, 3 * shards // 2)),
            pltpu.VMEM((2, rows, features), jnp.bfloat16),
            pltpu.VMEM((rows, height), jnp.bfloat16),
            pltpu.VMEM((depth, rows, width), jnp.float32),
            pltpu.VMEM((rows, width), jnp.bfloat16),
            pltpu.SemaphoreType.DMA((2, CHUNKS, shards)),
            pltpu.SemaphoreType.DMA((2, CHUNKS, 4 * depth)),
            pltpu.VMEM((2, depth, rows, width), jnp.bfloat16),
            pltpu.VMEM((2, depth, rows, width), jnp.bfloat16),
            pltpu.SemaphoreType.DMA((2, CHUNKS, depth)),
            pltpu.SemaphoreType.DMA((2, CHUNKS, depth)),
            pltpu.VMEM((2, depth, rows, width), jnp.bfloat16),
            pltpu.VMEM((2, 2, depth, rows, width), jnp.bfloat16),
            pltpu.SemaphoreType.DMA((2, CHUNKS, depth)),
            pltpu.SemaphoreType.DMA((2, CHUNKS, 2, depth)),
            pltpu.SemaphoreType.DMA((1,)),
            pltpu.VMEM((6,) + trained[0].shape, jnp.float32),
            pltpu.VMEM((6, trained[0].shape[1], LANES), jnp.bfloat16),
            pltpu.SemaphoreType.DMA((6,)),
        ],
        compiler_params=pltpu.CompilerParams(collective_id=0, has_side_effects=True, vmem_limit_bytes=42 << 20),
    )(prompt, *gains, *trained)
    return write_out(outs)


D = 2048
FF = 5632


norm_eps = 1e-06


def add_products(columns_in, w_gate, w_up):
    widened = columns_in.astype(jnp.float32)
    dims = (((1,), (1,)), ((), ()))
    return (
        lax.dot_general(columns_in, w_gate, dims, preferred_element_type=jnp.float32),
        lax.dot_general(columns_in, w_up, dims, preferred_element_type=jnp.float32),
        jnp.sum(widened * widened, axis=1),
    )


def half_step(tokens, w_gate, w_up, w_down):
    gate_sum, up_sum, squares = add_products(
        lax.all_gather(tokens, "fs", axis=1, tiled=True), w_gate, w_up
    )
    row_scale = (lax.rsqrt(squares / D + norm_eps) * D ** (-0.5))[:, None]
    hidden = (jax.nn.silu(gate_sum * row_scale) * (up_sum * row_scale)).astype(jnp.bfloat16)
    partial_value = jnp.dot(hidden, w_down, preferred_element_type=jnp.float32)
    summed = lax.psum_scatter(
        partial_value.astype(jnp.bfloat16), "fs", scatter_dimension=1, tiled=True
    ).astype(jnp.float32)
    return (tokens.astype(jnp.float32) + 0.5 * FF ** (-0.5) * summed).astype(jnp.bfloat16)


def restore_rows(matrix, groups, shards, lanes):
    row_total, col_total = matrix.shape
    sub_rows = row_total // (groups * shards * lanes)
    shaped = matrix.reshape(groups, lanes, shards, sub_rows, col_total)
    return jnp.transpose(shaped, (0, 2, 1, 3, 4)).reshape(row_total, col_total)


def relayout(matrices):
    crossed = (
        lax.all_to_all(
            lax.all_to_all(matrices[0], "tp", split_axis=0, concat_axis=1, tiled=True),
            "fs",
            split_axis=1,
            concat_axis=0,
            tiled=True,
        ),
        lax.all_to_all(
            lax.all_to_all(matrices[1], "tp", split_axis=0, concat_axis=1, tiled=True),
            "fs",
            split_axis=1,
            concat_axis=0,
            tiled=True,
        ),
        lax.all_to_all(
            lax.all_to_all(matrices[2], "tp", split_axis=0, concat_axis=1, tiled=True),
            "fs",
            split_axis=1,
            concat_axis=0,
            tiled=True,
        ),
        lax.all_to_all(
            lax.all_to_all(matrices[3], "tp", split_axis=0, concat_axis=1, tiled=True),
            "fs",
            split_axis=1,
            concat_axis=0,
            tiled=True,
        ),
        lax.all_to_all(
            lax.all_to_all(matrices[4], "tp", split_axis=0, concat_axis=1, tiled=True),
            "fs",
            split_axis=1,
            concat_axis=0,
            tiled=True,
        ),
        lax.all_to_all(
            lax.all_to_all(matrices[5], "tp", split_axis=0, concat_axis=1, tiled=True),
            "fs",
            split_axis=1,
            concat_axis=0,
            tiled=True,
        ),
    )
    gathered = (
        lax.all_gather(crossed[0], ("gr", "tp"), axis=0, tiled=True),
        lax.all_gather(crossed[1], ("gr", "tp"), axis=0, tiled=True),
        lax.all_gather(crossed[2], ("gr", "tp"), axis=0, tiled=True),
        lax.all_gather(crossed[3], ("gr", "tp"), axis=0, tiled=True),
        lax.all_gather(crossed[4], ("gr", "tp"), axis=0, tiled=True),
        lax.all_gather(crossed[5], ("gr", "tp"), axis=0, tiled=True),
    )
    groups = lax.axis_size("gr")
    shards = lax.axis_size("fs")
    lanes = lax.axis_size("tp")
    return tuple((restore_rows(matrix, groups, shards, lanes).T for matrix in gathered))


def direct_fits(token_shape, shape):
    shards = lax.axis_size("fs")
    units = shape[1] * lax.axis_size("tp")
    whole_rows = shape[0] == LANES and shape[1] % LANES == 0 and units % (16 * shards) == 0
    whole_tokens = token_shape[0] % (32 * CHUNKS) == 0 and token_shape[1] % LANES == 0
    pairs = shards % 4 == 0 and lax.axis_size("gr") == 2 and lax.axis_size("tp") == 2
    return whole_rows and whole_tokens and pairs


def local(prompt, gain_pre, gate_pre, up_pre, down_pre, gain_post, gate_post, up_post, down_post):
    rounded = (
        (gain_pre[:, None] * gate_pre).astype(jnp.bfloat16),
        (gain_pre[:, None] * up_pre).astype(jnp.bfloat16),
        down_pre.astype(jnp.bfloat16),
        (gain_post[:, None] * gate_post).astype(jnp.bfloat16),
        (gain_post[:, None] * up_post).astype(jnp.bfloat16),
        down_post.astype(jnp.bfloat16),
    )
    if direct_fits(prompt.shape, gate_pre.shape):
        trained = (gate_pre, up_pre, down_pre, gate_post, up_post, down_post)
        gains = (gain_pre[None, :], gain_post[None, :])
        return tuple(whole(prompt, gains, trained, lax.axis_size("fs")))
    served = relayout(rounded)
    middle = half_step(prompt, served[0], served[1], served[2])
    result = half_step(middle, served[3], served[4], served[5])
    return (result, served[0], served[1], served[2], served[3], served[4], served[5])


def solution(mesh):
    placed = (
        P(("gr", "tp"), "fs"),
        P(("gr", "fs")),
        P(("gr", "fs"), "tp"),
        P(("gr", "fs"), "tp"),
        P(("gr", "fs"), "tp"),
        P(("gr", "fs")),
        P(("gr", "fs"), "tp"),
        P(("gr", "fs"), "tp"),
        P(("gr", "fs"), "tp"),
    )
    return jax.shard_map(
        local,
        mesh=mesh,
        in_specs=placed,
        out_specs=(
            P(("gr", "tp"), "fs"),
            P("fs", None),
            P("fs", None),
            P("fs", None),
            P("fs", None),
            P("fs", None),
            P("fs", None),
        ),
        check_vma=False,
    )
```

```python
import functools

import jax
import jax.numpy as jnp
from jax import lax
from jax.experimental import pallas as pl
from jax.experimental.pallas import tpu as pltpu
from jax.sharding import PartitionSpec as P

MESH = pl.DeviceIdType.MESH
LANES = 128


def lanes_of(block, width):
    return pl.ds(pl.multiple_of(block * width, width), width)


def place_of(count, here, k):
    low = here < count // 2
    z = jnp.where(low, here, count - 1 - here)
    j = k - (count - 1 - 2 * z)
    late = jnp.maximum(j, 0)
    nearby = z + (1 - 2 * lax.rem(late, 2)) * (z - late // 2)
    found = jnp.where(j < 0, count - 1 - k, nearby)
    return jnp.where(low, found, count - 1 - found)


class HandOver:
    def __init__(self, shards, sources, held, land, first, onward):
        self.n, self.half = shards, shards // 2
        self.sources, self.held = sources, held
        self.land, self.first, self.onward = land, first, onward
        self.g, self.f, self.t = lax.axis_index("gr"), lax.axis_index("fs"), lax.axis_index("tp")
        self.height = held[0].shape[0]

    def slot(self, m, column):
        return self.held[m].at[:, lanes_of(column, LANES)]

    def copy(self, m, column, source, send, target):
        return pltpu.make_async_remote_copy(
            src_ref=source,
            dst_ref=self.slot(m, column),
            send_sem=send,
            recv_sem=self.land.at[m, column],
            device_id=target,
            device_id_type=MESH,
        )

    def outgoing(self, m, k, act):
        home = lax.rem(self.f, 2)
        target = self.t * self.half + k
        column = self.g * self.n + self.f
        block = self.sources[m].at[pl.ds(pl.multiple_of(k * self.height, 16), self.height), :]
        stays = jnp.logical_and(target == self.f, home == self.t)

        @pl.when(jnp.logical_not(stays))
        def _():
            act(self.copy(m, column, block, self.first.at[m, k], (self.g, target, home)))

        return stays, column, block

    def send(self, m, k):
        stays, column, block = self.outgoing(m, k, lambda c: c.start())

        @pl.when(stays)
        def _():
            pltpu.make_async_copy(block, self.slot(m, column), self.land.at[m, column]).start()

    def arrived(self, m, column):
        slot = self.slot(m, column)
        pltpu.make_async_copy(slot, slot, self.land.at[m, column]).wait()

    def forward(self, m, i, column, which):
        target = (1 - self.g, self.f, self.t) if which == 0 else (self.g, self.f, 1 - self.t)
        return self.copy(m, column, self.slot(m, column), self.onward.at[m, which * self.half + i], target)

    def near(self, i):
        return self.g * self.n + 2 * i + self.t

    def far(self, i):
        return (1 - self.g) * self.n + 2 * i + self.t

    def relay_near(self, m, j):
        i = place_of(self.half, self.f // 2, self.half - 1 - j)
        self.arrived(m, self.near(i))
        self.forward(m, i, self.near(i), 0).start()
        self.forward(m, i, self.near(i), 1).start()

    def relay_far(self, m, j):
        i = place_of(self.half, self.f // 2, self.half - 1 - j)
        self.arrived(m, self.far(i))
        self.forward(m, i, self.far(i), 2).start()

    def settle(self, m):
        for group in range(2):
            for i in range(self.half):
                self.arrived(m, group * self.n + 2 * i + 1 - self.t)

    def drain(self, m):
        for k in range(self.half):
            self.outgoing(m, k, lambda c: c.wait_send())
        for i in range(self.half):
            self.forward(m, i, self.near(i), 0).wait_send()
            self.forward(m, i, self.near(i), 1).wait_send()
            self.forward(m, i, self.far(i), 2).wait_send()


def greet(shards):
    g, f, t = lax.axis_index("gr"), lax.axis_index("fs"), lax.axis_index("tp")
    barrier = pltpu.get_barrier_semaphore()
    for step in range(1, 2 * shards):
        place = lax.rem(2 * f + t + step, 2 * shards)
        pl.semaphore_signal(barrier, inc=1, device_id=(g, place // 2, lax.rem(place, 2)), device_id_type=MESH)
    pl.semaphore_signal(barrier, inc=1, device_id=(1 - g, f, t), device_id_type=MESH)
    return lambda: pl.semaphore_wait(barrier, 2 * shards)


CHUNKS = 4
PLACES = 4


def chunks_of(h):
    return range(h * CHUNKS // 2, (h + 1) * CHUNKS // 2)


def half_of(h, rows):
    return pl.ds(h * rows // 2, rows // 2)


class Tokens:
    def __init__(self, shards, step, x, gathered, gather_out, over_y, into_y, y_out, y_in, over_z, into_z, z_out, z_in):
        self.n, self.depth = shards, shards // 2
        self.x, self.gathered, self.gather_out = x.at[step], gathered.at[step], gather_out.at[step]
        self.over_y, self.into_y, self.y_out, self.y_in = over_y.at[step], into_y.at[step], y_out.at[step], y_in.at[step]
        self.over_z, self.into_z, self.z_out, self.z_in = over_z.at[step], into_z.at[step], z_out.at[step], z_in.at[step]
        self.g, self.f, self.t = lax.axis_index("gr"), lax.axis_index("fs"), lax.axis_index("tp")
        self.z, self.y = self.f // 2, lax.rem(self.f, 2)
        self.width = over_y.shape[-1]
        self.rows = x.shape[1] // CHUNKS
        self.sent = []

    def span(self, c):
        return pl.ds(c * self.rows, self.rows)

    def go(self, when, make):
        @pl.when(when)
        def _():
            make().start()

        self.sent.append((when, make))

    def copy(self, source, dest, send, recv, target):
        return pltpu.make_async_remote_copy(
            src_ref=source,
            dst_ref=dest,
            send_sem=send,
            recv_sem=recv,
            device_id=(self.g, target, self.t),
            device_id_type=MESH,
        )

    def piece(self, owner, c):
        return self.x.at[self.span(c), lanes_of(owner, self.width)]

    def hand_on(self, when, source, owner, sem, target, c):
        self.go(when, lambda: self.copy(source(), self.piece(owner, c), self.gather_out.at[c, sem], self.gathered.at[c, owner], target))

    def spread(self, own, c):
        source = own.at[self.span(c), :]
        self.hand_on(self.z < self.depth - 1, lambda: source, self.f, 0, self.f + 2, c)
        self.hand_on(self.z > 0, lambda: source, self.f, 1, self.f - 2, c)
        self.hand_on(self.z >= 0, lambda: source, self.f, 2, 2 * self.z + 1 - self.y, c)

    def came(self, owner, c):
        piece = self.piece(owner, c)
        pltpu.make_async_copy(piece, piece, self.gathered.at[c, owner]).wait()

    def pass_on(self, i, c):
        for side, sign in enumerate((-1, 1)):
            place = self.z + sign * (1 + i)
            owner = 2 * place + self.y
            there = jnp.logical_and(place >= 0, place < self.depth)
            further = jnp.logical_and(there, self.z < self.depth - 1 if sign < 0 else self.z > 0)
            sem = 3 + 4 * i + 2 * side

            @pl.when(there)
            def _(owner=owner):
                self.came(owner, c)

            self.hand_on(further, lambda owner=owner: self.piece(owner, c), owner, sem, self.f - 2 * sign, c)
            self.hand_on(there, lambda owner=owner: self.piece(owner, c), owner, sem + 1, 2 * self.z + 1 - self.y, c)

    def collect(self, h):
        for i in range(self.depth):
            for c in chunks_of(h):
                self.came(2 * i + 1 - self.y, c)

    def activate(self, w_gate, w_up, hidden, features, h):
        span = half_of(h, self.x.shape[0])
        tokens = self.x[span, :]
        widened = tokens.astype(jnp.float32)
        squares = jnp.sum(widened * widened, axis=1, keepdims=True)
        scale = lax.rsqrt(squares / features + norm_eps) * features ** (-0.5)
        dims = (((1,), (1,)), ((), ()))
        gate = lax.dot_general(tokens, w_gate[...], dims, preferred_element_type=jnp.float32) * scale
        up = lax.dot_general(tokens, w_up[...], dims, preferred_element_type=jnp.float32) * scale
        hidden[span, :] = (gate / (1.0 + jnp.exp(-gate)) * up).astype(jnp.bfloat16)

    def term(self, hidden, w_down, owner):
        return jnp.dot(hidden[...], w_down[:, lanes_of(owner, self.width)], preferred_element_type=jnp.float32)

    def place(self, k):
        return place_of(self.depth, self.z, k)

    def swap(self, hidden, w_down, k, h):
        span = half_of(h, self.x.shape[0])
        self.over_y[k, span] = self.term(hidden.at[span, :], w_down, 2 * self.place(k) + 1 - self.y).astype(jnp.bfloat16)
        for c in chunks_of(h):
            part = (k, self.span(c))
            self.go(
                self.z >= 0,
                lambda c=c, part=part: self.copy(self.over_y.at[part], self.into_y.at[part], self.y_out.at[c, k], self.y_in.at[c, k], 2 * self.z + 1 - self.y),
            )

    def gather_term(self, hidden, w_down, own, k):
        own[k] = self.term(hidden, w_down, 2 * self.place(k) + self.y)

    def reduce(self, own, k, c):
        place = self.place(k)
        up = place > self.z
        side = jnp.where(up, 0, 1)
        inner = jnp.where(up, self.z, self.depth - 1 - self.z) > 0
        part = (k, self.span(c))
        passed = (side, place, self.span(c))
        self.wait(self.into_y.at[part], self.y_in.at[c, k])

        @pl.when(inner)
        def _():
            self.wait(self.into_z.at[passed], self.z_in.at[c, side, place])
            total = own[part] + self.into_y[part].astype(jnp.float32) + self.into_z[passed].astype(jnp.float32)
            self.over_z[part] = total.astype(jnp.bfloat16)

        @pl.when(jnp.logical_not(inner))
        def _():
            self.over_z[part] = (own[part] + self.into_y[part].astype(jnp.float32)).astype(jnp.bfloat16)

        self.go(
            self.z >= 0,
            lambda: self.copy(
                self.over_z.at[part],
                self.into_z.at[passed],
                self.z_out.at[c, k],
                self.z_in.at[c, side, place],
                self.f + 2 - 4 * side,
            ),
        )

    def wait(self, landed, sem):
        pltpu.make_async_copy(landed, landed, sem).wait()

    def finish(self, own, units, c):
        k = self.depth - 1
        part = (k, self.span(c))
        self.wait(self.into_y.at[part], self.y_in.at[c, k])
        own[part] += self.into_y[part].astype(jnp.float32)
        for side in range(2):
            inner = self.z > 0 if side == 0 else self.z < self.depth - 1

            @pl.when(inner)
            def _(side=side):
                passed = (side, self.z, self.span(c))
                self.wait(self.into_z.at[passed], self.z_in.at[c, side, self.z])
                own[part] += self.into_z[passed].astype(jnp.float32)

        before = self.x[self.span(c), lanes_of(self.f, self.width)].astype(jnp.float32)
        return (before + 0.5 * units ** (-0.5) * own[part]).astype(jnp.bfloat16)

    def drain(self):
        for when, make in self.sent:

            @pl.when(when)
            def _(make=make):
                make().wait_send()


def whole_kernel(shards, features, units, *refs):
    prompt, gains, trained, result, held = refs[0], refs[1:3], refs[3:9], refs[9], refs[10:16]
    land, first, onward, x, hidden, own, middle = refs[16:23]
    traffic, alone, raw, turned, loaded = refs[23:33], refs[33], refs[34], refs[35], refs[36]
    sources = [turned.at[m] for m in range(6)]
    loads = [pltpu.make_async_copy(trained[m], raw.at[m], loaded.at[m]) for m in range(6)]
    moves = HandOver(shards, sources, held, land, first, onward)
    half = shards // 2
    tokens = [Tokens(shards, step, x, *traffic) for step in range(2)]

    def prepare(m):
        loads[m].wait()
        for c in range(raw.shape[2] // LANES):
            span = pl.ds(c * LANES, LANES)
            block = raw[m, :, span].T
            if m % 3 < 2:
                block = block * gains[m // 3][...]
            turned[m, span, :] = block.astype(jnp.bfloat16)

    def send(m):
        for k in range(half):
            moves.send(m, k)

    row = lax.rem(moves.f, 2)
    turning = row != moves.t

    def send_turning(m):
        for j in range(half // 2):
            moves.send(m, 2 * j + 1 - row)

    def send_straight(m):
        for j in range(half // 2):
            moves.send(m, 2 * j + row)

    def near_if(m, turned_row):
        @pl.when(turning if turned_row else jnp.logical_not(turning))
        def _():
            for i in range(half):
                moves.relay_near(m, i)

    def far_if(m, turned_row):
        @pl.when(turning if turned_row else jnp.logical_not(turning))
        def _():
            for i in range(half):
                moves.relay_far(m, i)

    def spread(step, own_tokens):
        for c in range(CHUNKS):
            tokens[step].spread(own_tokens, c)

    def pass_on(step, i):
        for c in range(CHUNKS):
            tokens[step].pass_on(i, c)

    def collect(step, h):
        tokens[step].collect(h)

    def activate(step, h):
        tokens[step].activate(held[3 * step], held[3 * step + 1], hidden, features, h)

    def swap(step, k, h):
        tokens[step].swap(hidden, held[3 * step + 2], k, h)

    def terms(step):
        for k in range(half):
            tokens[step].gather_term(hidden, held[3 * step + 2], own, k)

    def reduce(step, k, h):
        for c in chunks_of(h):
            tokens[step].reduce(own, k, c)

    def hand_back():
        for c in range(CHUNKS):
            span = tokens[0].span(c)
            done = tokens[0].finish(own, units, c)
            middle[span, :] = done
            x[1, span, lanes_of(tokens[1].f, tokens[1].width)] = done
            tokens[1].spread(middle, c)

    def deliver():
        for c in range(CHUNKS):
            result[tokens[1].span(c), :] = tokens[1].finish(own, units, c)

    for load in loads:
        load.start()
    ready = greet(shards)
    prepare(0)
    ready()
    start = pltpu.make_async_copy(prompt, x.at[0, :, lanes_of(moves.f, prompt.shape[1])], alone.at[0])
    start.start()
    spread(0, prompt)
    moves.send(0, 0)
    moves.send(0, 1)
    moves.send(0, 2)
    moves.send(0, 3)
    prepare(1)
    prepare(2)
    prepare(3)
    prepare(4)
    prepare(5)
    pass_on(0, 0)
    moves.send(1, 0)
    moves.send(1, 1)
    moves.relay_near(0, 0)
    moves.relay_near(0, 1)
    moves.relay_near(0, 2)
    pass_on(0, 1)
    moves.relay_near(0, 3)
    moves.send(1, 2)
    moves.send(1, 3)
    moves.relay_near(1, 0)
    moves.relay_near(1, 1)
    moves.relay_near(1, 2)
    moves.send(2, 0)
    moves.send(2, 1)
    pass_on(0, 2)
    moves.relay_near(1, 3)
    moves.send(2, 2)
    moves.send(2, 3)
    moves.relay_far(0, 0)
    moves.relay_far(0, 1)
    moves.relay_far(0, 2)
    moves.relay_far(0, 3)
    moves.relay_near(2, 0)
    moves.relay_near(2, 1)
    moves.relay_near(2, 2)
    moves.send(3, 0)
    moves.send(3, 1)
    moves.send(3, 2)
    moves.send(3, 3)
    moves.send(4, 0)
    moves.send(4, 1)
    moves.send(4, 2)
    moves.send(4, 3)
    moves.relay_near(2, 3)
    moves.relay_far(1, 0)
    moves.relay_far(1, 1)
    moves.relay_far(1, 2)
    moves.relay_far(1, 3)
    start.wait()
    collect(0, 0)
    collect(0, 1)
    moves.settle(0)
    moves.settle(1)
    moves.send(5, 0)
    moves.send(5, 1)
    moves.send(5, 2)
    moves.send(5, 3)
    activate(0, 0)
    activate(0, 1)
    moves.relay_far(2, 0)
    moves.relay_far(2, 1)
    moves.relay_far(2, 2)
    moves.relay_far(2, 3)
    moves.settle(2)
    swap(0, 0, 0)
    swap(0, 0, 1)
    swap(0, 1, 0)
    swap(0, 1, 1)
    swap(0, 2, 0)
    swap(0, 2, 1)
    swap(0, 3, 0)
    swap(0, 3, 1)
    terms(0)
    moves.relay_near(3, 0)
    moves.relay_near(3, 1)
    moves.relay_near(3, 2)
    moves.relay_near(3, 3)
    reduce(0, 0, 0)
    reduce(0, 0, 1)
    reduce(0, 1, 0)
    reduce(0, 1, 1)
    moves.relay_near(4, 0)
    moves.relay_near(4, 1)
    moves.relay_near(4, 2)
    moves.relay_near(4, 3)
    reduce(0, 2, 0)
    reduce(0, 2, 1)
    hand_back()
    moves.relay_far(3, 0)
    moves.relay_far(3, 1)
    moves.relay_far(3, 2)
    moves.relay_far(3, 3)
    moves.relay_near(5, 0)
    moves.relay_near(5, 1)
    moves.relay_near(5, 2)
    moves.relay_near(5, 3)
    pass_on(1, 0)
    moves.relay_far(4, 0)
    moves.relay_far(4, 1)
    moves.relay_far(4, 2)
    moves.relay_far(4, 3)
    pass_on(1, 1)
    moves.relay_far(5, 0)
    moves.relay_far(5, 1)
    moves.relay_far(5, 2)
    moves.relay_far(5, 3)
    pass_on(1, 2)
    collect(1, 0)
    moves.settle(3)
    moves.settle(4)
    activate(1, 0)
    moves.settle(5)
    swap(1, 0, 0)
    collect(1, 1)
    activate(1, 1)
    swap(1, 0, 1)
    swap(1, 1, 0)
    swap(1, 1, 1)
    swap(1, 2, 0)
    swap(1, 2, 1)
    swap(1, 3, 0)
    swap(1, 3, 1)
    terms(1)
    reduce(1, 0, 0)
    reduce(1, 0, 1)
    reduce(1, 1, 0)
    reduce(1, 1, 1)
    reduce(1, 2, 0)
    reduce(1, 2, 1)
    deliver()
    for m in range(6):
        moves.drain(m)
    for part in tokens:
        part.drain()


def write_kernel(count, *refs):
    sources, outs, written = refs[:count], refs[count : 2 * count], refs[2 * count]
    copies = [pltpu.make_async_copy(sources[i], outs[i], written.at[i]) for i in range(count)]
    for copy in copies:
        copy.start()
    for copy in copies:
        copy.wait()


def write_out(arrays):
    count = len(arrays)
    return pl.pallas_call(
        functools.partial(write_kernel, count),
        out_shape=[jax.ShapeDtypeStruct(a.shape, a.dtype) for a in arrays],
        in_specs=[pl.BlockSpec(memory_space=pltpu.VMEM)] * count,
        out_specs=[pl.BlockSpec(memory_space=pl.ANY)] * count,
        scratch_shapes=[pltpu.SemaphoreType.DMA((count,))],
        compiler_params=pltpu.CompilerParams(vmem_limit_bytes=1 << 20),
    )(*[pltpu.with_memory_space_constraint(a, pltpu.VMEM) for a in arrays])


def whole(prompt, gains, trained, shards):
    units = trained[0].shape[1] * lax.axis_size("tp")
    height = units // shards
    features = LANES * lax.axis_size("gr") * shards
    rows, width = prompt.shape
    depth = shards // 2
    any_space = pl.BlockSpec(memory_space=pl.ANY)
    vmem = pl.BlockSpec(memory_space=pltpu.VMEM)
    outs = pl.pallas_call(
        functools.partial(whole_kernel, shards, features, units),
        out_shape=[pltpu.VMEM(prompt.shape, jnp.bfloat16)] + [pltpu.VMEM((height, features), jnp.bfloat16)] * 6,
        in_specs=[any_space] + [vmem] * 2 + [any_space] * 6,
        out_specs=[vmem] * 7,
        scratch_shapes=[
            pltpu.SemaphoreType.DMA((6, 2 * shards)),
            pltpu.SemaphoreType.DMA((6, shards // 2)),
            pltpu.SemaphoreType.DMA((6, 3 * shards // 2)),
            pltpu.VMEM((2, rows, features), jnp.bfloat16),
            pltpu.VMEM((rows, height), jnp.bfloat16),
            pltpu.VMEM((depth, rows, width), jnp.float32),
            pltpu.VMEM((rows, width), jnp.bfloat16),
            pltpu.SemaphoreType.DMA((2, CHUNKS, shards)),
            pltpu.SemaphoreType.DMA((2, CHUNKS, 4 * depth)),
            pltpu.VMEM((2, depth, rows, width), jnp.bfloat16),
            pltpu.VMEM((2, depth, rows, width), jnp.bfloat16),
            pltpu.SemaphoreType.DMA((2, CHUNKS, depth)),
            pltpu.SemaphoreType.DMA((2, CHUNKS, depth)),
            pltpu.VMEM((2, depth, rows, width), jnp.bfloat16),
            pltpu.VMEM((2, 2, depth, rows, width), jnp.bfloat16),
            pltpu.SemaphoreType.DMA((2, CHUNKS, depth)),
            pltpu.SemaphoreType.DMA((2, CHUNKS, 2, depth)),
            pltpu.SemaphoreType.DMA((1,)),
            pltpu.VMEM((6,) + trained[0].shape, jnp.float32),
            pltpu.VMEM((6, trained[0].shape[1], LANES), jnp.bfloat16),
            pltpu.SemaphoreType.DMA((6,)),
        ],
        compiler_params=pltpu.CompilerParams(collective_id=0, has_side_effects=True, vmem_limit_bytes=42 << 20),
    )(prompt, *gains, *trained)
    return write_out(outs)


D = 2048
FF = 5632


norm_eps = 1e-06


def add_products(columns_in, w_gate, w_up):
    widened = columns_in.astype(jnp.float32)
    dims = (((1,), (1,)), ((), ()))
    return (
        lax.dot_general(columns_in, w_gate, dims, preferred_element_type=jnp.float32),
        lax.dot_general(columns_in, w_up, dims, preferred_element_type=jnp.float32),
        jnp.sum(widened * widened, axis=1),
    )


def half_step(tokens, w_gate, w_up, w_down):
    gate_sum, up_sum, squares = add_products(
        lax.all_gather(tokens, "fs", axis=1, tiled=True), w_gate, w_up
    )
    row_scale = (lax.rsqrt(squares / D + norm_eps) * D ** (-0.5))[:, None]
    hidden = (jax.nn.silu(gate_sum * row_scale) * (up_sum * row_scale)).astype(jnp.bfloat16)
    partial_value = jnp.dot(hidden, w_down, preferred_element_type=jnp.float32)
    summed = lax.psum_scatter(
        partial_value.astype(jnp.bfloat16), "fs", scatter_dimension=1, tiled=True
    ).astype(jnp.float32)
    return (tokens.astype(jnp.float32) + 0.5 * FF ** (-0.5) * summed).astype(jnp.bfloat16)


def restore_rows(matrix, groups, shards, lanes):
    row_total, col_total = matrix.shape
    sub_rows = row_total // (groups * shards * lanes)
    shaped = matrix.reshape(groups, lanes, shards, sub_rows, col_total)
    return jnp.transpose(shaped, (0, 2, 1, 3, 4)).reshape(row_total, col_total)


def relayout(matrices):
    crossed = (
        lax.all_to_all(
            lax.all_to_all(matrices[0], "tp", split_axis=0, concat_axis=1, tiled=True),
            "fs",
            split_axis=1,
            concat_axis=0,
            tiled=True,
        ),
        lax.all_to_all(
            lax.all_to_all(matrices[1], "tp", split_axis=0, concat_axis=1, tiled=True),
            "fs",
            split_axis=1,
            concat_axis=0,
            tiled=True,
        ),
        lax.all_to_all(
            lax.all_to_all(matrices[2], "tp", split_axis=0, concat_axis=1, tiled=True),
            "fs",
            split_axis=1,
            concat_axis=0,
            tiled=True,
        ),
        lax.all_to_all(
            lax.all_to_all(matrices[3], "tp", split_axis=0, concat_axis=1, tiled=True),
            "fs",
            split_axis=1,
            concat_axis=0,
            tiled=True,
        ),
        lax.all_to_all(
            lax.all_to_all(matrices[4], "tp", split_axis=0, concat_axis=1, tiled=True),
            "fs",
            split_axis=1,
            concat_axis=0,
            tiled=True,
        ),
        lax.all_to_all(
            lax.all_to_all(matrices[5], "tp", split_axis=0, concat_axis=1, tiled=True),
            "fs",
            split_axis=1,
            concat_axis=0,
            tiled=True,
        ),
    )
    gathered = (
        lax.all_gather(crossed[0], ("gr", "tp"), axis=0, tiled=True),
        lax.all_gather(crossed[1], ("gr", "tp"), axis=0, tiled=True),
        lax.all_gather(crossed[2], ("gr", "tp"), axis=0, tiled=True),
        lax.all_gather(crossed[3], ("gr", "tp"), axis=0, tiled=True),
        lax.all_gather(crossed[4], ("gr", "tp"), axis=0, tiled=True),
        lax.all_gather(crossed[5], ("gr", "tp"), axis=0, tiled=True),
    )
    groups = lax.axis_size("gr")
    shards = lax.axis_size("fs")
    lanes = lax.axis_size("tp")
    return tuple((restore_rows(matrix, groups, shards, lanes).T for matrix in gathered))


def direct_fits(token_shape, shape):
    shards = lax.axis_size("fs")
    units = shape[1] * lax.axis_size("tp")
    whole_rows = shape[0] == LANES and shape[1] % LANES == 0 and units % (16 * shards) == 0
    whole_tokens = token_shape[0] % (32 * CHUNKS) == 0 and token_shape[1] % LANES == 0
    pairs = shards == 2 * PLACES and lax.axis_size("gr") == 2 and lax.axis_size("tp") == 2
    return whole_rows and whole_tokens and pairs


def local(prompt, gain_pre, gate_pre, up_pre, down_pre, gain_post, gate_post, up_post, down_post):
    rounded = (
        (gain_pre[:, None] * gate_pre).astype(jnp.bfloat16),
        (gain_pre[:, None] * up_pre).astype(jnp.bfloat16),
        down_pre.astype(jnp.bfloat16),
        (gain_post[:, None] * gate_post).astype(jnp.bfloat16),
        (gain_post[:, None] * up_post).astype(jnp.bfloat16),
        down_post.astype(jnp.bfloat16),
    )
    if direct_fits(prompt.shape, gate_pre.shape):
        trained = (gate_pre, up_pre, down_pre, gate_post, up_post, down_post)
        gains = (gain_pre[None, :], gain_post[None, :])
        return tuple(whole(prompt, gains, trained, lax.axis_size("fs")))
    served = relayout(rounded)
    middle = half_step(prompt, served[0], served[1], served[2])
    result = half_step(middle, served[3], served[4], served[5])
    return (result, served[0], served[1], served[2], served[3], served[4], served[5])


def solution(mesh):
    placed = (
        P(("gr", "tp"), "fs"),
        P(("gr", "fs")),
        P(("gr", "fs"), "tp"),
        P(("gr", "fs"), "tp"),
        P(("gr", "fs"), "tp"),
        P(("gr", "fs")),
        P(("gr", "fs"), "tp"),
        P(("gr", "fs"), "tp"),
        P(("gr", "fs"), "tp"),
    )
    return jax.shard_map(
        local,
        mesh=mesh,
        in_specs=placed,
        out_specs=(
            P(("gr", "tp"), "fs"),
            P("fs", None),
            P("fs", None),
            P("fs", None),
            P("fs", None),
            P("fs", None),
            P("fs", None),
        ),
        check_vma=False,
    )
```
